256 devices in a mesh: fs: 32 (over z, x), tp: 8 (over y, core).
Axes of the slice: x: 4, y: 4, z: 8, core: 2. Of those that a mesh axis runs over, the one named last changes fastest.
Arguments:
- tokens: bfloat16 [4096, 2048], P('fs'), may hold values from -6 to 6
- route_ids: int32 [4096, 2], P('fs'), may hold values from 0 to 63, as said below
- route_weights: float32 [4096, 2], P('fs'), may hold values from 0.05 to 0.6
- norm_gain: float32 [2048], P('fs'), may hold values from 0.1 to 1.9
- gate_weight: float32 [64, 2048, 1024], P(None, 'fs', 'tp'), may hold values from -6 to 6
- up_weight: float32 [64, 2048, 1024], P(None, 'fs', 'tp'), may hold values from -6 to 6
- down_weight: float32 [64, 2048, 1024], P(None, 'fs', 'tp'), may hold values from -6 to 6
Outputs:
- gate_served: bfloat16 [64, 2048, 1024], P('fs', None, 'tp')
- up_served: bfloat16 [64, 2048, 1024], P('fs', None, 'tp')
- down_served: bfloat16 [64, 2048, 1024], P('fs', None, 'tp')
- combined: bfloat16 [4096, 2048], P('fs', 'tp')
The draws below stay inside these ranges and needn't reach their ends.
Inputs may be any that keep to these rules, and one draw needn't show every extreme that they name: `route_ids`: each row names 2 different experts of one group, numbers g * 16 to g * 16 + 15 for some g. In each aligned block of 128 rows (the rows of one index of fs) no expert is named by more than 8 rows, and some experts are named by exactly 8 rows in every block.
All inputs are finite; a program needn't handle non-finite values.
Results may differ from the reference program's by a relative error of at most 0.015.
Values may be sent and summed in bfloat16 or wider, within the bound.
No kernel may reach another device: no remote copies, remote signals or barrier semaphores. Data moves between devices by JAX's collectives and lax.ppermute only.
A program may use at most 64 MiB of HBM per device.

```python
import jax
import jax.numpy as jnp
from jax import lax

D = 2048
H = 1024
GROUPS = 4
TOP = 2
TOK_DEV = 128
EXPERTS = 64
CAP = 8
TOKENS = 4096
N_TP = 8


def shuffle_table(table_key):
    return jax.random.permutation(table_key, EXPERTS // GROUPS)


def draw_route_ids(key, part):
    per_group = EXPERTS // GROUPS
    heavy_group = jax.random.randint(jax.random.fold_in(key, 11), (), 0, GROUPS)

    def one_block(block_number):
        block_key = jax.random.fold_in(jax.random.fold_in(key, 23), block_number)
        shuffled = jax.random.permutation(jax.random.fold_in(block_key, 1), TOK_DEV)
        other_shift = jax.random.randint(jax.random.fold_in(block_key, 2), (TOK_DEV,), 1, GROUPS)
        ranked = jnp.zeros((TOK_DEV,), jnp.int32).at[shuffled].set(jnp.arange(TOK_DEV, dtype=jnp.int32))
        group_ids = jnp.where(ranked < TOK_DEV // 2, heavy_group, (heavy_group + other_shift) % GROUPS)
        onehot = (group_ids[:, None] == jnp.arange(GROUPS, dtype=jnp.int32)[None, :]).astype(jnp.int32)
        rank_in = jnp.sum((jnp.cumsum(onehot, axis=0) - onehot) * onehot, axis=1)
        offsets = jax.random.randint(jax.random.fold_in(block_key, 3), (GROUPS,), 0, per_group)
        tables = jax.vmap(shuffle_table)(jax.random.split(jax.random.fold_in(block_key, 4), GROUPS))
        position = 2 * rank_in + jnp.sum(onehot * offsets[None, :], axis=1)
        first_slot = position % per_group
        second_slot = (position + 1) % per_group
        row_table = tables[group_ids]
        pick_first = jnp.take_along_axis(row_table, first_slot[:, None], axis=1)
        pick_second = jnp.take_along_axis(row_table, second_slot[:, None], axis=1)
        return jnp.concatenate([pick_first, pick_second], axis=1) + group_ids[:, None] * per_group
    blocks = jax.vmap(one_block)(jnp.arange(TOKENS // TOK_DEV, dtype=jnp.int32))
    return blocks.reshape(TOKENS, TOP).astype(jnp.int32)


def block_levels(stream_key, dims, cuts, least, largest):
    factor_of = 1.0
    for dim, blocks in cuts:
        draws = jax.random.uniform(jax.random.fold_in(jax.random.fold_in(stream_key, 6), dim), (blocks,), jnp.float32, least / len(cuts), largest / len(cuts))
        factor_of = factor_of * jnp.repeat(jnp.exp(draws), dims[dim] // blocks).reshape((-1,) + (1,) * (len(dims) - 1 - dim))
    return factor_of


def bell_draw(stream_key, shape, deviation, reach, cuts=(), kind=jnp.bfloat16):
    array = jax.random.normal(stream_key, shape, jnp.float32) * deviation
    if len(cuts) > 0:
        array = block_levels(stream_key, shape, cuts, -0.22, 0.18) * array
    return jnp.clip(array, min=-reach, max=reach).astype(kind)


def setup_inputs(seed: int = 0) -> dict:
    key_list = jax.random.split(jax.random.key(seed), 8)
    return {
        "tokens": bell_draw(key_list[0], (TOKENS, D), 1.0, 6.0, ((0, 32),)),
        "route_ids": draw_route_ids(jax.random.fold_in(key_list[7], 71), 0),
        "route_weights": jnp.clip(0.05 + 0.55 * jax.random.uniform(key_list[2], (TOKENS, TOP), jnp.float32) ** block_levels(key_list[2], (TOKENS, TOP), ((0, 32),), -0.2, 0.2), 0.05, 0.6),
        "norm_gain": jnp.clip(1.0 + 0.18 * jax.random.normal(key_list[3], (D,), jnp.float32), 0.1, 1.9),
        "gate_weight": bell_draw(key_list[4], (EXPERTS, D, H), 1.0, 6.0, ((1, 32), (2, 8)), jnp.float32),
        "up_weight": bell_draw(key_list[5], (EXPERTS, D, H), 1.0, 6.0, ((1, 32), (2, 8)), jnp.float32),
        "down_weight": bell_draw(key_list[6], (EXPERTS, D, H), 1.0, 6.0, ((1, 32), (2, 8)), jnp.float32),
    }


epsilon = 1e-06

def slot_positions(route_ids):
    blocked = route_ids.reshape(TOKENS // TOK_DEV, TOK_DEV * TOP)
    onehot = (blocked[:, :, None] == jnp.arange(EXPERTS, dtype=jnp.int32)[None, None, :]).astype(jnp.int32)
    earlier = jnp.cumsum(onehot, axis=1) - onehot
    return lax.optimization_barrier(jnp.sum(earlier * onehot, axis=2)).reshape(TOKENS, TOP).astype(jnp.int32)

def reference(tokens, route_ids, route_weights, norm_gain, gate_weight, up_weight, down_weight):
    scaling = norm_gain[:, None]
    gate_served = (scaling * gate_weight).astype(jnp.bfloat16)
    up_served = (scaling * up_weight).astype(jnp.bfloat16)
    down_served = down_weight.astype(jnp.bfloat16)
    widened = tokens.astype(jnp.float32)
    normed = (widened * lax.rsqrt(lax.optimization_barrier(jnp.mean(widened * widened, axis=1, keepdims=True)) + epsilon)).astype(jnp.bfloat16)
    block_index = (jnp.arange(TOKENS, dtype=jnp.int32) // TOK_DEV)[:, None]
    slot_index = (block_index * CAP + slot_positions(route_ids)).astype(jnp.int32)
    slot_rows = TOKENS // TOK_DEV * CAP
    token_of = jnp.broadcast_to(jnp.arange(TOKENS, dtype=jnp.int32)[:, None], (TOKENS, TOP))
    row_owner = jnp.zeros((EXPERTS, slot_rows), jnp.int32).at[route_ids, slot_index].set(token_of)

    def expert(operands):
        gate_one, up_one, down_one, owners = operands
        inputs = normed[owners]
        gate_pre = jnp.dot(inputs, gate_one, preferred_element_type=jnp.float32) * D ** (-0.5)
        up_pre = jnp.dot(inputs, up_one, preferred_element_type=jnp.float32) * D ** (-0.5)
        hidden = (jax.nn.silu(gate_pre) * up_pre).astype(jnp.bfloat16)
        blocks_h = hidden.astype(jnp.float32).reshape(slot_rows, N_TP, H // N_TP)
        blocks_d = down_one.astype(jnp.float32).reshape(D, N_TP, H // N_TP)
        partial_value = (jnp.einsum('rtj,dtj->trd', blocks_h, blocks_d) * H ** (-0.5)).astype(jnp.bfloat16)
        return lax.optimization_barrier(jnp.sum(partial_value.astype(jnp.float32), axis=0)).astype(jnp.bfloat16)
    expert_outs = lax.map(expert, (gate_served, up_served, down_served, row_owner))
    picked = expert_outs[route_ids, slot_index].astype(jnp.float32)
    combined = lax.optimization_barrier(jnp.sum(route_weights[:, :, None] * picked, axis=1))
    return (gate_served, up_served, down_served, combined.astype(jnp.bfloat16))
```

```python
import jax
import jax.numpy as jnp
from jax import lax
from jax.sharding import Mesh
from jax.sharding import PartitionSpec as P

GROUPS = 4
TP = ("tp_0", "tp_1")
epsilon = 1e-06
BF16 = jnp.bfloat16
F32 = jnp.float32


def exchange(blocks, axis):
    return lax.all_to_all(blocks, axis, split_axis=0, concat_axis=0, tiled=True)


def spread_over_tp(blocks):
    n = blocks.shape[0]
    me = lax.axis_index(TP)
    result = blocks
    for d in range(1, n):
        other = me ^ d
        sent = lax.dynamic_index_in_dim(blocks, other, 0, keepdims=True)
        got = lax.ppermute(sent, TP, [(i, i ^ d) for i in range(n)])
        result = lax.dynamic_update_index_in_dim(result, got, other, 0)
    return result


def body(tokens, route_ids, route_weights, norm_gain, gate_weight, up_weight, down_weight):
    tok_rows, d_model = tokens.shape
    experts, rows_here, hidden_local = gate_weight.shape
    sources = lax.axis_size("fs")
    n_tp = lax.axis_size(TP)
    per_device = experts // sources
    capacity = tok_rows * GROUPS // experts
    col_width = d_model // n_tp
    slots = sources * capacity
    slots_out = per_device * capacity

    widened = tokens.astype(F32)
    inverse = lax.rsqrt(jnp.mean(widened * widened, axis=1, keepdims=True) + epsilon)
    own = lax.dynamic_slice_in_dim(tokens, lax.axis_index(TP) * col_width, col_width, 1)
    own = (own.astype(F32) * inverse).astype(BF16)
    slot = lax.broadcasted_iota(jnp.int32, (1, experts * capacity), 1)
    expert_of, slot_of = slot // capacity, slot % capacity
    picks = [route_ids[:, k : k + 1] == expert_of for k in range(route_ids.shape[1])]
    named = picks[0]
    for p in picks[1:]:
        named = named | p
    row = lax.broadcasted_iota(jnp.int32, (tok_rows, tok_rows), 0)
    col = lax.broadcasted_iota(jnp.int32, (tok_rows, tok_rows), 1)
    before = jnp.dot((row > col).astype(BF16), named.astype(BF16), preferred_element_type=F32)
    here = named & (before == slot_of.astype(F32))
    dispatched = lax.dot_general(
        here.astype(BF16), own, (((0,), (0,)), ((), ())), preferred_element_type=F32
    ).astype(BF16)
    weight = sum(
        jnp.where(p & here, route_weights[:, k : k + 1], 0.0) for k, p in enumerate(picks)
    )

    down_cast = jnp.concatenate(
        [down_weight[e::per_device].astype(BF16) for e in range(per_device)], axis=2
    )
    first = jnp.concatenate([dispatched.reshape(sources, slots_out, col_width), down_cast], axis=1)
    with jax.named_scope("ex_first"):
        first = exchange(first, "fs")
    arrived = first[:, :slots_out].reshape(sources, per_device, capacity, col_width)
    down_both = first[:, slots_out:].reshape(d_model, per_device * hidden_local)
    down_served = jnp.stack(
        [down_both[:, e * hidden_local : (e + 1) * hidden_local] for e in range(per_device)]
    )

    scaling = norm_gain[None, :, None]
    folded = jnp.concatenate(
        [
            (scaling * w[e::per_device]).astype(BF16)
            for e in range(per_device)
            for w in (gate_weight, up_weight)
        ],
        axis=2,
    )
    folded, first_done = lax.optimization_barrier((folded, down_both))
    with jax.named_scope("ex_second"):
        both = exchange(folded, "fs").reshape(d_model, 2 * per_device * hidden_local)
    parts = [both[:, i * hidden_local : (i + 1) * hidden_local] for i in range(2 * per_device)]
    gate_served = jnp.stack(parts[0::2])
    up_served = jnp.stack(parts[1::2])

    with jax.named_scope("down_tp"):
        down_tp = spread_over_tp(first_done.reshape(n_tp, col_width, per_device * hidden_local))
    half = col_width // 2
    outs = []
    for e in range(per_device):
        share = arrived[:, e].reshape(slots, col_width)
        with jax.named_scope("tok_tp"):
            pieces = [
                lax.all_gather(share[:, h * half : (h + 1) * half], TP, axis=0) for h in range(2)
            ]
        both_e = both[:, 2 * e * hidden_local : 2 * (e + 1) * hidden_local]
        x = jnp.concatenate(pieces, axis=2).transpose(1, 0, 2).reshape(slots, d_model)
        pre = jnp.dot(x, both_e, preferred_element_type=F32) * (d_model ** (-0.5))
        hidden = (jax.nn.silu(pre[:, :hidden_local]) * pre[:, hidden_local:]).astype(BF16)
        with jax.named_scope("hid_tp"):
            whole = lax.all_gather(hidden, TP, axis=0)
        down_here = down_tp[:, :, e * hidden_local : (e + 1) * hidden_local]
        out = jnp.einsum("bsu,biu->si", whole, down_here, preferred_element_type=F32)
        outs.append((out * ((hidden_local * n_tp) ** (-0.5))).astype(BF16))
    back = jnp.stack([o.reshape(sources, capacity, col_width) for o in outs], axis=1)
    with jax.named_scope("ex_back"):
        back = exchange(back.reshape(sources, slots_out, col_width), "fs")
    back = back.reshape(experts * capacity, col_width)
    combined = jnp.dot(weight, back.astype(F32), precision=lax.Precision.HIGHEST)
    return (gate_served, up_served, down_served, combined.astype(BF16))


def solution(mesh):
    torus = Mesh(mesh.devices.reshape(mesh.shape["fs"], 4, 2), ("fs", "tp_0", "tp_1"))
    return jax.shard_map(
        body,
        mesh=torus,
        in_specs=(
            P("fs", None),
            P("fs", None),
            P("fs", None),
            P("fs"),
            P(None, "fs", TP),
            P(None, "fs", TP),
            P(None, "fs", TP),
        ),
        out_specs=(P("fs", None, TP), P("fs", None, TP), P("fs", None, TP), P("fs", TP)),
        check_vma=False,
    )
```

```python
import jax
import jax.numpy as jnp
from jax import lax
from jax.sharding import Mesh
from jax.sharding import PartitionSpec as P

GROUPS = 4
TP = ("tp_0", "tp_1")
epsilon = 1e-06
BF16 = jnp.bfloat16
F32 = jnp.float32


def exchange(blocks, axis):
    return lax.all_to_all(blocks, axis, split_axis=0, concat_axis=0, tiled=True)


def steps():
    return [(s, r) for s in range(lax.axis_size("tp_0")) for r in range(lax.axis_size("tp_1"))]


def moved(x, s, r):
    ny, nc = lax.axis_size("tp_0"), lax.axis_size("tp_1")
    pairs = [(y * nc + c, ((y + s) % ny) * nc + (c ^ r)) for y in range(ny) for c in range(nc)]
    return lax.ppermute(x, TP, pairs)


def spread_over_tp(blocks):
    y, c = lax.axis_index("tp_0"), lax.axis_index("tp_1")
    ny, nc = lax.axis_size("tp_0"), lax.axis_size("tp_1")
    result = []
    for s, r in steps():
        sent = lax.dynamic_index_in_dim(blocks, (y + s) % ny * nc + (c ^ r), 0, keepdims=False)
        result.append(sent if (s, r) == (0, 0) else moved(sent, s, r))
    return result


def gathered_over_tp(x):
    result = []
    for s in range(lax.axis_size("tp_0")):
        same = x if s == 0 else moved(x, s, 0)
        result += [same, moved(same, 0, 1)]
    return result


def in_tp_order(pieces):
    y, c = lax.axis_index("tp_0"), lax.axis_index("tp_1")
    ny, nc = lax.axis_size("tp_0"), lax.axis_size("tp_1")
    result = jnp.zeros((ny * nc, *pieces[0].shape), pieces[0].dtype)
    for (s, r), piece in zip(steps(), pieces):
        place = (y - s) % ny * nc + (c ^ r)
        result = lax.dynamic_update_index_in_dim(result, piece, place, 0)
    return result


def body(tokens, route_ids, route_weights, norm_gain, gate_weight, up_weight, down_weight):
    tok_rows, d_model = tokens.shape
    experts, rows_here, hidden_local = gate_weight.shape
    sources = lax.axis_size("fs")
    n_tp = lax.axis_size(TP)
    per_device = experts // sources
    capacity = tok_rows * GROUPS // experts
    col_width = d_model // n_tp
    slots = sources * capacity
    slots_out = per_device * capacity

    widened = tokens.astype(F32)
    inverse = lax.rsqrt(jnp.mean(widened * widened, axis=1, keepdims=True) + epsilon)
    own = lax.dynamic_slice_in_dim(tokens, lax.axis_index(TP) * col_width, col_width, 1)
    own = (own.astype(F32) * inverse).astype(BF16)
    slot = lax.broadcasted_iota(jnp.int32, (1, experts * capacity), 1)
    expert_of, slot_of = slot // capacity, slot % capacity
    picks = [route_ids[:, k : k + 1] == expert_of for k in range(route_ids.shape[1])]
    named = picks[0]
    for p in picks[1:]:
        named = named | p
    row = lax.broadcasted_iota(jnp.int32, (tok_rows, tok_rows), 0)
    col = lax.broadcasted_iota(jnp.int32, (tok_rows, tok_rows), 1)
    before = jnp.dot((row > col).astype(BF16), named.astype(BF16), preferred_element_type=F32)
    here = named & (before == slot_of.astype(F32))
    dispatched = lax.dot_general(
        here.astype(BF16), own, (((0,), (0,)), ((), ())), preferred_element_type=F32
    ).astype(BF16)
    weight = sum(
        jnp.where(p & here, route_weights[:, k : k + 1], 0.0) for k, p in enumerate(picks)
    )

    down_cast = jnp.concatenate(
        [down_weight[e::per_device].astype(BF16) for e in range(per_device)], axis=2
    )
    first = jnp.concatenate([dispatched.reshape(sources, slots_out, col_width), down_cast], axis=1)
    with jax.named_scope("ex_first"):
        first = exchange(first, "fs")
    arrived = first[:, :slots_out].reshape(sources, per_device, capacity, col_width)
    down_both = first[:, slots_out:].reshape(d_model, per_device * hidden_local)
    down_served = jnp.stack(
        [down_both[:, e * hidden_local : (e + 1) * hidden_local] for e in range(per_device)]
    )

    scaling = norm_gain[None, :, None]
    folded = jnp.concatenate(
        [
            (scaling * w[e::per_device]).astype(BF16)
            for e in range(per_device)
            for w in (gate_weight, up_weight)
        ],
        axis=2,
    )
    folded, first_done = lax.optimization_barrier((folded, down_both))
    with jax.named_scope("ex_second"):
        both = exchange(folded, "fs").reshape(d_model, 2 * per_device * hidden_local)
    parts = [both[:, i * hidden_local : (i + 1) * hidden_local] for i in range(2 * per_device)]
    gate_served = jnp.stack(parts[0::2])
    up_served = jnp.stack(parts[1::2])

    with jax.named_scope("down_tp"):
        down_tp = spread_over_tp(first_done.reshape(n_tp, col_width, per_device * hidden_local))
    share = arrived.transpose(1, 0, 2, 3).reshape(per_device * slots, col_width)
    with jax.named_scope("tok_tp"):
        x = in_tp_order(gathered_over_tp(share))
    hidden = []
    for e in range(per_device):
        both_e = both[:, 2 * e * hidden_local : 2 * (e + 1) * hidden_local]
        pre = jnp.einsum(
            "bsd,bdh->sh",
            x[:, e * slots : (e + 1) * slots],
            both_e.reshape(n_tp, col_width, 2 * hidden_local),
            preferred_element_type=F32,
        ) * (d_model ** (-0.5))
        hidden.append((jax.nn.silu(pre[:, :hidden_local]) * pre[:, hidden_local:]).astype(BF16))
    with jax.named_scope("hid_tp"):
        whole = jnp.concatenate(gathered_over_tp(jnp.concatenate(hidden, axis=0)), axis=1)
    outs = []
    for e in range(per_device):
        down_here = jnp.concatenate(
            [d[:, e * hidden_local : (e + 1) * hidden_local] for d in down_tp], axis=1
        )
        out = lax.dot_general(
            whole[e * slots : (e + 1) * slots],
            down_here,
            (((1,), (1,)), ((), ())),
            preferred_element_type=F32,
        )
        outs.append((out * ((hidden_local * n_tp) ** (-0.5))).astype(BF16))
    back = jnp.stack([o.reshape(sources, capacity, col_width) for o in outs], axis=1)
    with jax.named_scope("ex_back"):
        back = exchange(back.reshape(sources, slots_out, col_width), "fs")
    back = back.reshape(experts * capacity, col_width)
    combined = jnp.dot(weight, back.astype(F32), precision=lax.Precision.HIGHEST)
    return (gate_served, up_served, down_served, combined.astype(BF16))


def solution(mesh):
    torus = Mesh(mesh.devices.reshape(mesh.shape["fs"], 4, 2), ("fs", "tp_0", "tp_1"))
    return jax.shard_map(
        body,
        mesh=torus,
        in_specs=(
            P("fs", None),
            P("fs", None),
            P("fs", None),
            P("fs"),
            P(None, "fs", TP),
            P(None, "fs", TP),
            P(None, "fs", TP),
        ),
        out_specs=(P("fs", None, TP), P("fs", None, TP), P("fs", None, TP), P("fs", TP)),
        check_vma=False,
    )
```

```python
import jax
import jax.numpy as jnp
from jax import lax
from jax.experimental import pallas as pl
from jax.experimental.pallas import tpu as pltpu
from jax.sharding import Mesh
from jax.sharding import PartitionSpec as P

GROUPS = 4
TP = ("tp_0", "tp_1")
epsilon = 1e-06
BF16 = jnp.bfloat16
F32 = jnp.float32
MIB = 1024 * 1024


def exchange(blocks, axis):
    return lax.all_to_all(blocks, axis, split_axis=0, concat_axis=0, tiled=True)


def steps():
    return [(s, r) for s in range(lax.axis_size("tp_0")) for r in range(lax.axis_size("tp_1"))]


def moved(x, s, r):
    ny, nc = lax.axis_size("tp_0"), lax.axis_size("tp_1")
    pairs = [(y * nc + c, ((y + s) % ny) * nc + (c ^ r)) for y in range(ny) for c in range(nc)]
    return lax.ppermute(x, TP, pairs)


def spread_over_tp(blocks):
    y, c = lax.axis_index("tp_0"), lax.axis_index("tp_1")
    ny, nc = lax.axis_size("tp_0"), lax.axis_size("tp_1")
    result = []
    for s, r in steps():
        sent = lax.dynamic_index_in_dim(blocks, (y + s) % ny * nc + (c ^ r), 0, keepdims=False)
        result.append(sent if (s, r) == (0, 0) else moved(sent, s, r))
    return result


def gathered_over_tp(x):
    result = []
    for s in range(lax.axis_size("tp_0")):
        same = x if s == 0 else moved(x, s, 0)
        result += [same, moved(same, 0, 1)]
    return result


def prelude(tokens, route_ids, route_weights, down_weight, sources, n_tp):
    tok_rows, d_model = tokens.shape
    experts, rows_here, hidden_local = down_weight.shape
    per_device = experts // sources
    capacity = tok_rows * GROUPS // experts
    slots_out = per_device * capacity
    width = d_model // n_tp
    parts = 2
    dests = sources // parts
    slots = dests * slots_out

    def kernel(me_ref, tok_ref, own_ref, ids_ref, w_ref, down_ref, out_ref, weight_ref, own_scr):
        g = pl.program_id(0)

        @pl.when(g == 0)
        def _():
            x = tok_ref[...].astype(F32)
            inverse = lax.rsqrt(jnp.mean(x * x, axis=1, keepdims=True) + epsilon)
            own_scr[...] = (own_ref[...].astype(F32) * inverse).astype(BF16)

        slot = lax.broadcasted_iota(jnp.int32, (slots, tok_rows), 0) + g * slots
        expert_of, slot_of = slot // capacity, slot % capacity
        picks = [ids_ref[k : k + 1, :] == expert_of for k in range(ids_ref.shape[0])]
        named = picks[0]
        for p in picks[1:]:
            named = named | p
        row = lax.broadcasted_iota(jnp.int32, (tok_rows, tok_rows), 0)
        col = lax.broadcasted_iota(jnp.int32, (tok_rows, tok_rows), 1)
        earlier = jnp.where(row < col, 1.0, 0.0).astype(BF16)
        named_one = jnp.where(named, 1.0, 0.0).astype(BF16)
        before = jnp.dot(named_one, earlier, preferred_element_type=F32)
        here = named & (before == slot_of.astype(F32))
        here_one = jnp.where(here, 1.0, 0.0).astype(BF16)
        sent = jnp.dot(here_one, own_scr[...], preferred_element_type=F32).astype(BF16)
        out_ref[:, :slots_out, :] = sent.reshape(dests, slots_out, width)
        weight = jnp.zeros((slots, tok_rows), F32)
        for k, p in enumerate(picks):
            weight = weight + jnp.where(p & here, w_ref[k : k + 1, :], 0.0)
        weight_ref[...] = weight
        down = down_ref[...].astype(BF16).reshape(dests, per_device, rows_here, hidden_local)
        for e in range(per_device):
            out_ref[:, slots_out:, e * hidden_local : (e + 1) * hidden_local] = down[:, e]

    routes = route_ids.shape[1]
    grid = pltpu.PrefetchScalarGridSpec(
        num_scalar_prefetch=1,
        grid=(parts,),
        in_specs=[
            pl.BlockSpec((tok_rows, d_model), lambda g, me: (0, 0)),
            pl.BlockSpec((tok_rows, width), lambda g, me: (0, me[0])),
            pl.BlockSpec((routes, tok_rows), lambda g, me: (0, 0)),
            pl.BlockSpec((routes, tok_rows), lambda g, me: (0, 0)),
            pl.BlockSpec((dests * per_device, rows_here, hidden_local), lambda g, me: (g, 0, 0)),
        ],
        out_specs=[
            pl.BlockSpec((dests, slots_out + rows_here, width), lambda g, me: (g, 0, 0)),
            pl.BlockSpec((slots, tok_rows), lambda g, me: (g, 0)),
        ],
        scratch_shapes=[pltpu.VMEM((tok_rows, width), BF16)],
    )
    return pl.pallas_call(
        kernel,
        grid_spec=grid,
        out_shape=[
            pltpu.HBM((sources, slots_out + rows_here, width), BF16),
            pltpu.HBM((experts * capacity, tok_rows), F32),
        ],
        compiler_params=pltpu.CompilerParams(
            dimension_semantics=("arbitrary",), vmem_limit_bytes=12 * MIB
        ),
        name="prelude",
    )(
        lax.axis_index(TP).astype(jnp.int32).reshape(1),
        pltpu.with_memory_space_constraint(tokens, pltpu.HBM),
        pltpu.with_memory_space_constraint(tokens, pltpu.HBM),
        pltpu.with_memory_space_constraint(route_ids.T, pltpu.HBM),
        pltpu.with_memory_space_constraint(route_weights.T, pltpu.HBM),
        pltpu.with_memory_space_constraint(down_weight, pltpu.HBM),
    )


def hidden_units(pieces, both, per_device, capacity):
    sources, _, width = pieces[0].shape
    d_model, columns = both.shape
    slots = sources * capacity
    span = columns // per_device
    unit = span // 2
    order = steps()
    ny, nc = lax.axis_size("tp_0"), lax.axis_size("tp_1")

    def kernel(me_ref, both_ref, *refs):
        sources_ref, out_ref, held, sems = refs[: len(order)], refs[-3], refs[-2], refs[-1]
        copies = [
            pltpu.make_async_copy(piece, held.at[i], sems.at[i])
            for i, piece in enumerate(sources_ref)
        ]
        for copy in copies:
            copy.start()
        acc = [jnp.zeros((slots, span), F32) for _ in range(per_device)]
        for i, (s, r) in enumerate(order):
            copies[i].wait()
            block = lax.rem(me_ref[0] - s + ny, ny) * nc + (me_ref[1] if r == 0 else nc - 1 - me_ref[1])
            start = pl.multiple_of(block * width, width)
            for e in range(per_device):
                x = held[i, :, e * capacity : (e + 1) * capacity, :].reshape(slots, width)
                w = both_ref[pl.ds(start, width), e * span : (e + 1) * span]
                acc[e] = acc[e] + jnp.dot(x, w, preferred_element_type=F32)
        for e in range(per_device):
            pre = acc[e] * (d_model ** (-0.5))
            gate, up = pre[:, :unit], pre[:, unit:]
            out_ref[e * slots : (e + 1) * slots, :] = (gate / (1.0 + jnp.exp(-gate)) * up).astype(BF16)

    vmem = pl.BlockSpec(memory_space=pltpu.VMEM)
    me = jnp.stack([lax.axis_index("tp_0"), lax.axis_index("tp_1")]).astype(jnp.int32)
    return pl.pallas_call(
        kernel,
        in_specs=[pl.BlockSpec(memory_space=pltpu.SMEM), vmem]
        + [pl.BlockSpec(memory_space=pltpu.HBM)] * len(pieces),
        out_specs=vmem,
        scratch_shapes=[
            pltpu.VMEM((len(pieces), *pieces[0].shape), BF16),
            pltpu.SemaphoreType.DMA((len(pieces),)),
        ],
        out_shape=jax.ShapeDtypeStruct((per_device * slots, unit), BF16),
        compiler_params=pltpu.CompilerParams(vmem_limit_bytes=8 * MIB),
        name="hidden_units",
    )(me, both, *(pltpu.with_memory_space_constraint(p, pltpu.HBM) for p in pieces))


def down_projected(hidden, down, per_device, capacity, scale):
    rows, unit = hidden[0].shape
    width = down[0].shape[0]
    slots = rows // per_device
    sources = slots // capacity
    n = len(hidden)

    def kernel(*refs):
        h, d, out_ref = refs[:n], refs[n : 2 * n], refs[-1]
        for e in range(per_device):
            x = jnp.concatenate([ref[e * slots : (e + 1) * slots, :] for ref in h], axis=1)
            w = jnp.concatenate([ref[:, e * unit : (e + 1) * unit] for ref in d], axis=1)
            acc = lax.dot_general(x, w, (((1,), (1,)), ((), ())), preferred_element_type=F32)
            out_ref[:, e * capacity : (e + 1) * capacity, :] = (
                (acc * scale).astype(BF16).reshape(sources, capacity, width)
            )

    vmem = pl.BlockSpec(memory_space=pltpu.VMEM)
    return pl.pallas_call(
        kernel,
        in_specs=[vmem] * (2 * n),
        out_specs=vmem,
        out_shape=jax.ShapeDtypeStruct((sources, per_device * capacity, width), BF16),
        compiler_params=pltpu.CompilerParams(vmem_limit_bytes=8 * MIB),
        name="down_projected",
    )(*hidden, *down)


def work(tokens, route_ids, route_weights, norm_gain, gate_weight, up_weight, down_weight):
    tok_rows, d_model = tokens.shape
    experts, _, hidden_local = gate_weight.shape
    sources = lax.axis_size("fs")
    n_tp = lax.axis_size(TP)
    per_device = experts // sources
    capacity = tok_rows * GROUPS // experts
    col_width = d_model // n_tp
    slots_out = per_device * capacity

    first, weight = prelude(tokens, route_ids, route_weights, down_weight, sources, n_tp)
    first = exchange(first, "fs")

    scaling = norm_gain[None, :, None]
    folded = jnp.concatenate(
        [
            (scaling * w[e::per_device]).astype(BF16)
            for e in range(per_device)
            for w in (gate_weight, up_weight)
        ],
        axis=2,
    )
    folded, first = lax.optimization_barrier((folded, first))
    arrived = first[:, :slots_out]
    down_both = first[:, slots_out:].reshape(d_model, per_device * hidden_local)
    both = exchange(folded, "fs").reshape(d_model, 2 * per_device * hidden_local)

    down_tp = spread_over_tp(down_both.reshape(n_tp, col_width, per_device * hidden_local))
    pieces = gathered_over_tp(arrived)
    hidden = hidden_units(pieces, both, per_device, capacity)
    whole = gathered_over_tp(hidden)
    back = down_projected(whole, down_tp, per_device, capacity, (hidden_local * n_tp) ** (-0.5))
    back = exchange(back, "fs")
    back = back.reshape(experts * capacity, col_width).astype(F32)
    combined = lax.dot_general(
        weight, back, (((0,), (0,)), ((), ())), precision=lax.Precision.HIGHEST
    )
    parts = [both[:, i * hidden_local : (i + 1) * hidden_local] for i in range(2 * per_device)]
    down_served = jnp.stack(
        [down_both[:, e * hidden_local : (e + 1) * hidden_local] for e in range(per_device)]
    )
    return (jnp.stack(parts[0::2]), jnp.stack(parts[1::2]), down_served, combined.astype(BF16))


def solution(mesh):
    torus = Mesh(mesh.devices.reshape(mesh.shape["fs"], 4, 2), ("fs", "tp_0", "tp_1"))
    return jax.shard_map(
        work,
        mesh=torus,
        in_specs=(
            P("fs", None),
            P("fs", None),
            P("fs", None),
            P("fs"),
            P(None, "fs", TP),
            P(None, "fs", TP),
            P(None, "fs", TP),
        ),
        out_specs=(P("fs", None, TP), P("fs", None, TP), P("fs", None, TP), P("fs", TP)),
        check_vma=False,
    )
```

```python
import jax
import jax.numpy as jnp
from jax import lax
from jax.experimental import pallas as pl
from jax.experimental.pallas import tpu as pltpu
from jax.sharding import Mesh
from jax.sharding import PartitionSpec as P

GROUPS = 4
TP = ("tp_0", "tp_1")
epsilon = 1e-06
BF16 = jnp.bfloat16
F32 = jnp.float32
MIB = 1024 * 1024
FS_SHAPE = (8, 4)


def exchange(blocks, axis):
    return lax.all_to_all(blocks, axis, split_axis=0, concat_axis=0, tiled=True)


def steps():
    return [(s, r) for s in range(lax.axis_size("tp_0")) for r in range(lax.axis_size("tp_1"))]


def moved(x, s, r):
    ny, nc = lax.axis_size("tp_0"), lax.axis_size("tp_1")
    pairs = [(y * nc + c, ((y + s) % ny) * nc + (c ^ r)) for y in range(ny) for c in range(nc)]
    return lax.ppermute(x, TP, pairs)


def spread_over_tp(blocks):
    y, c = lax.axis_index("tp_0"), lax.axis_index("tp_1")
    ny, nc = lax.axis_size("tp_0"), lax.axis_size("tp_1")
    result = []
    for s, r in steps():
        sent = lax.dynamic_index_in_dim(blocks, (y + s) % ny * nc + (c ^ r), 0, keepdims=False)
        result.append(sent if (s, r) == (0, 0) else moved(sent, s, r))
    return result


def gathered_over_tp(x):
    result = []
    for s in range(lax.axis_size("tp_0")):
        same = x if s == 0 else moved(x, s, 0)
        result += [same, moved(same, 0, 1)]
    return result


def prelude(tokens, route_ids, route_weights, down_weight, sources, n_tp):
    tok_rows, d_model = tokens.shape
    experts, rows_here, hidden_local = down_weight.shape
    per_device = experts // sources
    capacity = tok_rows * GROUPS // experts
    slots_out = per_device * capacity
    width = d_model // n_tp
    parts = 2
    dests = sources // parts
    slots = dests * slots_out

    def kernel(me_ref, tok_ref, own_ref, ids_ref, w_ref, down_ref, out_ref, weight_ref, own_scr):
        g = pl.program_id(0)

        @pl.when(g == 0)
        def _():
            x = tok_ref[...].astype(F32)
            inverse = lax.rsqrt(jnp.mean(x * x, axis=1, keepdims=True) + epsilon)
            own_scr[...] = (own_ref[...].astype(F32) * inverse).astype(BF16)

        slot = lax.broadcasted_iota(jnp.int32, (slots, tok_rows), 0) + g * slots
        expert_of, slot_of = slot // capacity, slot % capacity
        picks = [ids_ref[k : k + 1, :] == expert_of for k in range(ids_ref.shape[0])]
        named = picks[0]
        for p in picks[1:]:
            named = named | p
        row = lax.broadcasted_iota(jnp.int32, (tok_rows, tok_rows), 0)
        col = lax.broadcasted_iota(jnp.int32, (tok_rows, tok_rows), 1)
        earlier = jnp.where(row < col, 1.0, 0.0).astype(BF16)
        named_one = jnp.where(named, 1.0, 0.0).astype(BF16)
        before = jnp.dot(named_one, earlier, preferred_element_type=F32)
        here = named & (before == slot_of.astype(F32))
        here_one = jnp.where(here, 1.0, 0.0).astype(BF16)
        sent = jnp.dot(here_one, own_scr[...], preferred_element_type=F32).astype(BF16)
        out_ref[:, :slots_out, :] = sent.reshape(dests, slots_out, width)
        weight = jnp.zeros((slots, tok_rows), F32)
        for k, p in enumerate(picks):
            weight = weight + jnp.where(p & here, w_ref[k : k + 1, :], 0.0)
        weight_ref[...] = weight
        down = down_ref[...].astype(BF16).reshape(dests, per_device, rows_here, hidden_local)
        for e in range(per_device):
            out_ref[:, slots_out:, e * hidden_local : (e + 1) * hidden_local] = down[:, e]

    routes = route_ids.shape[1]
    grid = pltpu.PrefetchScalarGridSpec(
        num_scalar_prefetch=1,
        grid=(parts,),
        in_specs=[
            pl.BlockSpec((tok_rows, d_model), lambda g, me: (0, 0)),
            pl.BlockSpec((tok_rows, width), lambda g, me: (0, me[0])),
            pl.BlockSpec((routes, tok_rows), lambda g, me: (0, 0)),
            pl.BlockSpec((routes, tok_rows), lambda g, me: (0, 0)),
            pl.BlockSpec((dests * per_device, rows_here, hidden_local), lambda g, me: (g, 0, 0)),
        ],
        out_specs=[
            pl.BlockSpec((dests, slots_out + rows_here, width), lambda g, me: (g, 0, 0)),
            pl.BlockSpec((slots, tok_rows), lambda g, me: (g, 0)),
        ],
        scratch_shapes=[pltpu.VMEM((tok_rows, width), BF16)],
    )
    return pl.pallas_call(
        kernel,
        grid_spec=grid,
        out_shape=[
            pltpu.HBM((sources, slots_out + rows_here, width), BF16),
            pltpu.HBM((experts * capacity, tok_rows), F32),
        ],
        compiler_params=pltpu.CompilerParams(
            dimension_semantics=("arbitrary",), vmem_limit_bytes=12 * MIB
        ),
        name="prelude",
    )(
        lax.axis_index(TP).astype(jnp.int32).reshape(1),
        pltpu.with_memory_space_constraint(tokens, pltpu.HBM),
        pltpu.with_memory_space_constraint(tokens, pltpu.HBM),
        pltpu.with_memory_space_constraint(route_ids.T, pltpu.HBM),
        pltpu.with_memory_space_constraint(route_weights.T, pltpu.HBM),
        pltpu.with_memory_space_constraint(down_weight, pltpu.HBM),
    )


def hidden_units(pieces, top, rest, per_device, capacity):
    sources, _, width = pieces[0].shape
    columns = top.shape[2]
    rows_here = top.shape[1] + rest.shape[1]
    d_model = sources * rows_here
    across = width // rows_here
    slots = sources * capacity
    span = columns // per_device
    unit = span // 2
    order = steps()
    ny, nc = lax.axis_size("tp_0"), lax.axis_size("tp_1")

    def kernel(me_ref, top_ref, rest_ref, *refs):
        sources_ref, out_ref, held, sems = refs[: len(order)], refs[-3], refs[-2], refs[-1]
        copies = [
            pltpu.make_async_copy(piece, held.at[i], sems.at[i])
            for i, piece in enumerate(sources_ref)
        ]
        for copy in copies:
            copy.start()
        acc = [jnp.zeros((slots, span), F32) for _ in range(per_device)]
        for i, (s, r) in enumerate(order):
            copies[i].wait()
            block = lax.rem(me_ref[0] - s + ny, ny) * nc + (me_ref[1] if r == 0 else nc - 1 - me_ref[1])
            here = pl.ds(block * across, across)
            for e in range(per_device):
                x = held[i, :, e * capacity : (e + 1) * capacity, :].reshape(slots, width)
                w = jnp.concatenate(
                    [ref[here, :, e * span : (e + 1) * span] for ref in (top_ref, rest_ref)], axis=1
                ).reshape(width, span)
                acc[e] = acc[e] + jnp.dot(x, w, preferred_element_type=F32)
        for e in range(per_device):
            pre = acc[e] * (d_model ** (-0.5))
            gate, up = pre[:, :unit], pre[:, unit:]
            out_ref[e * slots : (e + 1) * slots, :] = (gate / (1.0 + jnp.exp(-gate)) * up).astype(BF16)

    vmem = pl.BlockSpec(memory_space=pltpu.VMEM)
    me = jnp.stack([lax.axis_index("tp_0"), lax.axis_index("tp_1")]).astype(jnp.int32)
    return pl.pallas_call(
        kernel,
        in_specs=[pl.BlockSpec(memory_space=pltpu.SMEM), vmem, vmem]
        + [pl.BlockSpec(memory_space=pltpu.HBM)] * len(pieces),
        out_specs=vmem,
        scratch_shapes=[
            pltpu.VMEM((len(pieces), *pieces[0].shape), BF16),
            pltpu.SemaphoreType.DMA((len(pieces),)),
        ],
        out_shape=jax.ShapeDtypeStruct((per_device * slots, unit), BF16),
        compiler_params=pltpu.CompilerParams(vmem_limit_bytes=8 * MIB),
        name="hidden_units",
    )(me, top, rest, *(pltpu.with_memory_space_constraint(p, pltpu.HBM) for p in pieces))


def ahead_along_z(blocks, nz, nx):
    z = lax.axis_index("fs") // nx
    by_z = blocks.reshape(nz, nx, *blocks.shape[1:])
    result = []
    for d in range(nz):
        sent = lax.dynamic_index_in_dim(by_z, (z + d) % nz, 0, keepdims=False)
        pairs = [(a * nx + b, ((a + d) % nz) * nx + b) for a in range(nz) for b in range(nx)]
        result.append(sent if d == 0 else lax.ppermute(sent, "fs", pairs))
    return result


def then_along_x(pieces, nz, nx):
    x = lax.axis_index("fs") % nx
    result = []
    for d in range(nx):
        sent = jnp.stack(
            [lax.dynamic_index_in_dim(p, (x + d) % nx, 0, keepdims=False) for p in pieces]
        )
        pairs = [(a * nx + b, a * nx + (b + d) % nx) for a in range(nz) for b in range(nx)]
        result.append(sent if d == 0 else lax.ppermute(sent, "fs", pairs))
    return result


def sources_in_order(pieces, nz, nx):
    block = pieces[0].shape[1:]

    def kernel(me_ref, *refs):
        z, x = me_ref[0] // nx, me_ref[0] % nx
        for dx, ref in enumerate(refs[:-1]):
            for dz in range(nz):
                source = lax.rem(z - dz + nz, nz) * nx + lax.rem(x - dx + nx, nx)
                refs[-1][pl.ds(source, 1)] = ref[dz : dz + 1]

    vmem = pl.BlockSpec(memory_space=pltpu.VMEM)
    return pl.pallas_call(
        kernel,
        in_specs=[pl.BlockSpec(memory_space=pltpu.SMEM)] + [vmem] * nx,
        out_specs=vmem,
        out_shape=jax.ShapeDtypeStruct((nz * nx, *block), BF16),
        compiler_params=pltpu.CompilerParams(vmem_limit_bytes=8 * MIB),
        name="sources_in_order",
    )(lax.axis_index("fs").astype(jnp.int32).reshape(1), *pieces)


def down_projected(hidden, down, per_device, capacity, scale):
    rows, unit = hidden[0].shape
    width = down[0].shape[0]
    slots = rows // per_device
    sources = slots // capacity
    n = len(hidden)

    def kernel(*refs):
        h, d, out_ref = refs[:n], refs[n : 2 * n], refs[-1]
        for e in range(per_device):
            x = jnp.concatenate([ref[e * slots : (e + 1) * slots, :] for ref in h], axis=1)
            w = jnp.concatenate([ref[:, e * unit : (e + 1) * unit] for ref in d], axis=1)
            acc = lax.dot_general(x, w, (((1,), (1,)), ((), ())), preferred_element_type=F32)
            out_ref[:, e * capacity : (e + 1) * capacity, :] = (
                (acc * scale).astype(BF16).reshape(sources, capacity, width)
            )

    vmem = pl.BlockSpec(memory_space=pltpu.VMEM)
    return pl.pallas_call(
        kernel,
        in_specs=[vmem] * (2 * n),
        out_specs=vmem,
        out_shape=jax.ShapeDtypeStruct((sources, per_device * capacity, width), BF16),
        compiler_params=pltpu.CompilerParams(vmem_limit_bytes=8 * MIB),
        name="down_projected",
    )(*hidden, *down)


def work(tokens, route_ids, route_weights, norm_gain, gate_weight, up_weight, down_weight):
    tok_rows, d_model = tokens.shape
    experts, rows_here, hidden_local = gate_weight.shape
    sources = lax.axis_size("fs")
    n_tp = lax.axis_size(TP)
    per_device = experts // sources
    capacity = tok_rows * GROUPS // experts
    col_width = d_model // n_tp
    slots_out = per_device * capacity

    first, weight = prelude(tokens, route_ids, route_weights, down_weight, sources, n_tp)
    first = exchange(first, "fs")

    scaling = norm_gain[None, :, None]
    folded = jnp.concatenate(
        [
            (scaling * w[e::per_device]).astype(BF16)
            for e in range(per_device)
            for w in (gate_weight, up_weight)
        ],
        axis=2,
    )
    nz, nx = FS_SHAPE
    ahead = rows_here // 4
    early = ahead_along_z(folded[:, :ahead], nz, nx)
    later, first = lax.optimization_barrier((folded[:, ahead:], first))
    arrived = first[:, :slots_out]
    down_both = first[:, slots_out:].reshape(d_model, per_device * hidden_local)
    rest = exchange(later, "fs")
    early = then_along_x(early, nz, nx)
    top = sources_in_order(early, nz, nx)

    down_tp = spread_over_tp(down_both.reshape(n_tp, col_width, per_device * hidden_local))
    pieces = gathered_over_tp(arrived)
    hidden = hidden_units(pieces, top, rest, per_device, capacity)
    whole = gathered_over_tp(hidden)
    back = down_projected(whole, down_tp, per_device, capacity, (hidden_local * n_tp) ** (-0.5))
    back = exchange(back, "fs")
    back = back.reshape(experts * capacity, col_width).astype(F32)
    combined = lax.dot_general(
        weight, back, (((0,), (0,)), ((), ())), precision=lax.Precision.HIGHEST
    )
    both = jnp.concatenate([top, rest], axis=1).reshape(d_model, 2 * per_device * hidden_local)
    parts = [both[:, i * hidden_local : (i + 1) * hidden_local] for i in range(2 * per_device)]
    gate_served, up_served = jnp.stack(parts[0::2]), jnp.stack(parts[1::2])
    down_served = jnp.stack(
        [down_both[:, e * hidden_local : (e + 1) * hidden_local] for e in range(per_device)]
    )
    return (gate_served, up_served, down_served, combined.astype(BF16))


def solution(mesh):
    torus = Mesh(mesh.devices.reshape(mesh.shape["fs"], 4, 2), ("fs", "tp_0", "tp_1"))
    return jax.shard_map(
        work,
        mesh=torus,
        in_specs=(
            P("fs", None),
            P("fs", None),
            P("fs", None),
            P("fs"),
            P(None, "fs", TP),
            P(None, "fs", TP),
            P(None, "fs", TP),
        ),
        out_specs=(P("fs", None, TP), P("fs", None, TP), P("fs", None, TP), P("fs", TP)),
        check_vma=False,
    )
```

```python
import jax
import jax.numpy as jnp
from jax import lax
from jax.experimental import pallas as pl
from jax.experimental.pallas import tpu as pltpu
from jax.sharding import Mesh
from jax.sharding import PartitionSpec as P

GROUPS = 4
TP = ("tp_0", "tp_1")
epsilon = 1e-06
BF16 = jnp.bfloat16
F32 = jnp.float32
MIB = 1024 * 1024
FS_SHAPE = (8, 4)


def exchange(blocks, axis):
    return lax.all_to_all(blocks, axis, split_axis=0, concat_axis=0, tiled=True)


def steps():
    return [(s, r) for s in range(lax.axis_size("tp_0")) for r in range(lax.axis_size("tp_1"))]


def moved(x, s, r):
    ny, nc = lax.axis_size("tp_0"), lax.axis_size("tp_1")
    pairs = [(y * nc + c, ((y + s) % ny) * nc + (c ^ r)) for y in range(ny) for c in range(nc)]
    return lax.ppermute(x, TP, pairs)


def spread_over_tp(blocks):
    y, c = lax.axis_index("tp_0"), lax.axis_index("tp_1")
    ny, nc = lax.axis_size("tp_0"), lax.axis_size("tp_1")
    result = []
    for s, r in steps():
        sent = lax.dynamic_index_in_dim(blocks, (y + s) % ny * nc + (c ^ r), 0, keepdims=False)
        result.append(sent if (s, r) == (0, 0) else moved(sent, s, r))
    return result


def gathered_over_tp(x):
    result = []
    for s in range(lax.axis_size("tp_0")):
        same = x if s == 0 else moved(x, s, 0)
        result += [same, moved(same, 0, 1)]
    return result


def prelude(tokens, route_ids, route_weights, down_weight, sources, n_tp):
    tok_rows, d_model = tokens.shape
    experts, rows_here, hidden_local = down_weight.shape
    per_device = experts // sources
    capacity = tok_rows * GROUPS // experts
    slots_out = per_device * capacity
    width = d_model // n_tp
    parts = 2
    dests = sources // parts
    slots = dests * slots_out

    def kernel(me_ref, tok_ref, own_ref, ids_ref, w_ref, down_ref, out_ref, weight_ref, own_scr):
        g = pl.program_id(0)

        @pl.when(g == 0)
        def _():
            x = tok_ref[...].astype(F32)
            inverse = lax.rsqrt(jnp.mean(x * x, axis=1, keepdims=True) + epsilon)
            own_scr[...] = (own_ref[...].astype(F32) * inverse).astype(BF16)

        slot = lax.broadcasted_iota(jnp.int32, (slots, tok_rows), 0) + g * slots
        expert_of, slot_of = slot // capacity, slot % capacity
        picks = [ids_ref[k : k + 1, :] == expert_of for k in range(ids_ref.shape[0])]
        named = picks[0]
        for p in picks[1:]:
            named = named | p
        row = lax.broadcasted_iota(jnp.int32, (tok_rows, tok_rows), 0)
        col = lax.broadcasted_iota(jnp.int32, (tok_rows, tok_rows), 1)
        earlier = jnp.where(row < col, 1.0, 0.0).astype(BF16)
        named_one = jnp.where(named, 1.0, 0.0).astype(BF16)
        before = jnp.dot(named_one, earlier, preferred_element_type=F32)
        here = named & (before == slot_of.astype(F32))
        here_one = jnp.where(here, 1.0, 0.0).astype(BF16)
        sent = jnp.dot(here_one, own_scr[...], preferred_element_type=F32).astype(BF16)
        out_ref[:, :slots_out, :] = sent.reshape(dests, slots_out, width)
        weight = jnp.zeros((slots, tok_rows), F32)
        for k, p in enumerate(picks):
            weight = weight + jnp.where(p & here, w_ref[k : k + 1, :], 0.0)
        weight_ref[...] = weight
        down = down_ref[...].astype(BF16).reshape(dests, per_device, rows_here, hidden_local)
        for e in range(per_device):
            out_ref[:, slots_out:, e * hidden_local : (e + 1) * hidden_local] = down[:, e]

    routes = route_ids.shape[1]
    grid = pltpu.PrefetchScalarGridSpec(
        num_scalar_prefetch=1,
        grid=(parts,),
        in_specs=[
            pl.BlockSpec((tok_rows, d_model), lambda g, me: (0, 0)),
            pl.BlockSpec((tok_rows, width), lambda g, me: (0, me[0])),
            pl.BlockSpec((routes, tok_rows), lambda g, me: (0, 0)),
            pl.BlockSpec((routes, tok_rows), lambda g, me: (0, 0)),
            pl.BlockSpec((dests * per_device, rows_here, hidden_local), lambda g, me: (g, 0, 0)),
        ],
        out_specs=[
            pl.BlockSpec((dests, slots_out + rows_here, width), lambda g, me: (g, 0, 0)),
            pl.BlockSpec((slots, tok_rows), lambda g, me: (g, 0)),
        ],
        scratch_shapes=[pltpu.VMEM((tok_rows, width), BF16)],
    )
    return pl.pallas_call(
        kernel,
        grid_spec=grid,
        out_shape=[
            pltpu.HBM((sources, slots_out + rows_here, width), BF16),
            pltpu.HBM((experts * capacity, tok_rows), F32),
        ],
        compiler_params=pltpu.CompilerParams(
            dimension_semantics=("arbitrary",), vmem_limit_bytes=12 * MIB
        ),
        name="prelude",
    )(
        lax.axis_index(TP).astype(jnp.int32).reshape(1),
        pltpu.with_memory_space_constraint(tokens, pltpu.HBM),
        pltpu.with_memory_space_constraint(tokens, pltpu.HBM),
        pltpu.with_memory_space_constraint(route_ids.T, pltpu.HBM),
        pltpu.with_memory_space_constraint(route_weights.T, pltpu.HBM),
        pltpu.with_memory_space_constraint(down_weight, pltpu.HBM),
    )


def hidden_units(pieces, top, rest, per_device, capacity):
    sources, _, width = pieces[0].shape
    columns = top.shape[2]
    rows_here = top.shape[1] + rest.shape[1]
    d_model = sources * rows_here
    across = width // rows_here
    slots = sources * capacity
    span = columns // per_device
    unit = span // 2
    order = steps()
    ny, nc = lax.axis_size("tp_0"), lax.axis_size("tp_1")

    def kernel(me_ref, top_ref, rest_ref, *refs):
        sources_ref, out_ref, held, sems = refs[: len(order)], refs[-3], refs[-2], refs[-1]
        copies = [
            pltpu.make_async_copy(piece, held.at[i], sems.at[i])
            for i, piece in enumerate(sources_ref)
        ]
        for copy in copies:
            copy.start()
        acc = [jnp.zeros((slots, span), F32) for _ in range(per_device)]
        for i, (s, r) in enumerate(order):
            copies[i].wait()
            block = lax.rem(me_ref[0] - s + ny, ny) * nc + (me_ref[1] if r == 0 else nc - 1 - me_ref[1])
            here = pl.ds(block * across, across)
            for e in range(per_device):
                x = held[i, :, e * capacity : (e + 1) * capacity, :].reshape(slots, width)
                w = jnp.concatenate(
                    [ref[here, :, e * span : (e + 1) * span] for ref in (top_ref, rest_ref)], axis=1
                ).reshape(width, span)
                acc[e] = acc[e] + jnp.dot(x, w, preferred_element_type=F32)
        for e in range(per_device):
            pre = acc[e] * (d_model ** (-0.5))
            gate, up = pre[:, :unit], pre[:, unit:]
            out_ref[e * slots : (e + 1) * slots, :] = (gate / (1.0 + jnp.exp(-gate)) * up).astype(BF16)

    vmem = pl.BlockSpec(memory_space=pltpu.VMEM)
    me = jnp.stack([lax.axis_index("tp_0"), lax.axis_index("tp_1")]).astype(jnp.int32)
    return pl.pallas_call(
        kernel,
        in_specs=[pl.BlockSpec(memory_space=pltpu.SMEM), vmem, vmem]
        + [pl.BlockSpec(memory_space=pltpu.HBM)] * len(pieces),
        out_specs=vmem,
        scratch_shapes=[
            pltpu.VMEM((len(pieces), *pieces[0].shape), BF16),
            pltpu.SemaphoreType.DMA((len(pieces),)),
        ],
        out_shape=jax.ShapeDtypeStruct((per_device * slots, unit), BF16),
        compiler_params=pltpu.CompilerParams(vmem_limit_bytes=8 * MIB),
        name="hidden_units",
    )(me, top, rest, *(pltpu.with_memory_space_constraint(p, pltpu.HBM) for p in pieces))


def ahead_along_z(blocks, nz, nx):
    z = lax.axis_index("fs") // nx
    by_z = blocks.reshape(nz, nx, *blocks.shape[1:])
    result = []
    for d in range(nz):
        sent = lax.dynamic_index_in_dim(by_z, (z + d) % nz, 0, keepdims=False)
        pairs = [(a * nx + b, ((a + d) % nz) * nx + b) for a in range(nz) for b in range(nx)]
        result.append(sent if d == 0 else lax.ppermute(sent, "fs", pairs))
    return result


def by_column(pieces, nx):
    block = pieces[0].shape[1:]
    nz = len(pieces)

    def kernel(me_ref, *refs):
        for d, out_ref in enumerate(refs[nz:]):
            column = lax.rem(me_ref[0] + d, nx)
            for dz, ref in enumerate(refs[:nz]):
                out_ref[dz : dz + 1] = ref[pl.ds(column, 1)]

    vmem = pl.BlockSpec(memory_space=pltpu.VMEM)
    x = lax.axis_index("fs") % nx
    return pl.pallas_call(
        kernel,
        in_specs=[pl.BlockSpec(memory_space=pltpu.SMEM)] + [vmem] * nz,
        out_specs=[vmem] * nx,
        out_shape=[jax.ShapeDtypeStruct((nz, *block), BF16)] * nx,
        compiler_params=pltpu.CompilerParams(vmem_limit_bytes=8 * MIB),
        name="by_column",
    )(x.astype(jnp.int32).reshape(1), *pieces)


def then_along_x(pieces, nz, nx):
    result = []
    for d, sent in enumerate(pieces):
        pairs = [(a * nx + b, a * nx + (b + d) % nx) for a in range(nz) for b in range(nx)]
        result.append(sent if d == 0 else lax.ppermute(sent, "fs", pairs))
    return result


def sources_in_order(pieces, nz, nx):
    block = pieces[0].shape[1:]

    def kernel(me_ref, *refs):
        z, x = me_ref[0] // nx, me_ref[0] % nx
        for dx, ref in enumerate(refs[:-1]):
            for dz in range(nz):
                source = lax.rem(z - dz + nz, nz) * nx + lax.rem(x - dx + nx, nx)
                refs[-1][pl.ds(source, 1)] = ref[dz : dz + 1]

    vmem = pl.BlockSpec(memory_space=pltpu.VMEM)
    return pl.pallas_call(
        kernel,
        in_specs=[pl.BlockSpec(memory_space=pltpu.SMEM)] + [vmem] * nx,
        out_specs=vmem,
        out_shape=jax.ShapeDtypeStruct((nz * nx, *block), BF16),
        compiler_params=pltpu.CompilerParams(vmem_limit_bytes=8 * MIB),
        name="sources_in_order",
    )(lax.axis_index("fs").astype(jnp.int32).reshape(1), *pieces)


def down_projected(hidden, down, per_device, capacity, scale):
    rows, unit = hidden[0].shape
    width = down[0].shape[0]
    slots = rows // per_device
    sources = slots // capacity
    n = len(hidden)

    def kernel(*refs):
        h, d, out_ref = refs[:n], refs[n : 2 * n], refs[-1]
        for e in range(per_device):
            x = jnp.concatenate([ref[e * slots : (e + 1) * slots, :] for ref in h], axis=1)
            w = jnp.concatenate([ref[:, e * unit : (e + 1) * unit] for ref in d], axis=1)
            acc = lax.dot_general(x, w, (((1,), (1,)), ((), ())), preferred_element_type=F32)
            out_ref[:, e * capacity : (e + 1) * capacity, :] = (
                (acc * scale).astype(BF16).reshape(sources, capacity, width)
            )

    vmem = pl.BlockSpec(memory_space=pltpu.VMEM)
    return pl.pallas_call(
        kernel,
        in_specs=[vmem] * (2 * n),
        out_specs=vmem,
        out_shape=jax.ShapeDtypeStruct((sources, per_device * capacity, width), BF16),
        compiler_params=pltpu.CompilerParams(vmem_limit_bytes=8 * MIB),
        name="down_projected",
    )(*hidden, *down)


def work(tokens, route_ids, route_weights, norm_gain, gate_weight, up_weight, down_weight):
    tok_rows, d_model = tokens.shape
    experts, rows_here, hidden_local = gate_weight.shape
    sources = lax.axis_size("fs")
    n_tp = lax.axis_size(TP)
    per_device = experts // sources
    capacity = tok_rows * GROUPS // experts
    col_width = d_model // n_tp
    slots_out = per_device * capacity

    first, weight = prelude(tokens, route_ids, route_weights, down_weight, sources, n_tp)
    first = exchange(first, "fs")

    scaling = norm_gain[None, :, None]
    folded = jnp.concatenate(
        [
            (scaling * w[e::per_device]).astype(BF16)
            for e in range(per_device)
            for w in (gate_weight, up_weight)
        ],
        axis=2,
    )
    nz, nx = FS_SHAPE
    ahead = rows_here // 4
    early = ahead_along_z(folded[:, :ahead], nz, nx)
    later, first = lax.optimization_barrier((folded[:, ahead:], first))
    arrived = first[:, :slots_out]
    down_both = first[:, slots_out:].reshape(d_model, per_device * hidden_local)
    rest = exchange(later, "fs")
    early = by_column(early, nx)
    early = then_along_x(early, nz, nx)
    top = sources_in_order(early, nz, nx)

    down_tp = spread_over_tp(down_both.reshape(n_tp, col_width, per_device * hidden_local))
    pieces = gathered_over_tp(arrived)
    hidden = hidden_units(pieces, top, rest, per_device, capacity)
    whole = gathered_over_tp(hidden)
    back = down_projected(whole, down_tp, per_device, capacity, (hidden_local * n_tp) ** (-0.5))
    back = exchange(back, "fs")
    back = back.reshape(experts * capacity, col_width).astype(F32)
    combined = lax.dot_general(
        weight, back, (((0,), (0,)), ((), ())), precision=lax.Precision.HIGHEST
    )
    both = jnp.concatenate([top, rest], axis=1).reshape(d_model, 2 * per_device * hidden_local)
    parts = [both[:, i * hidden_local : (i + 1) * hidden_local] for i in range(2 * per_device)]
    gate_served, up_served = jnp.stack(parts[0::2]), jnp.stack(parts[1::2])
    down_served = jnp.stack(
        [down_both[:, e * hidden_local : (e + 1) * hidden_local] for e in range(per_device)]
    )
    return (gate_served, up_served, down_served, combined.astype(BF16))


def solution(mesh):
    torus = Mesh(mesh.devices.reshape(mesh.shape["fs"], 4, 2), ("fs", "tp_0", "tp_1"))
    return jax.shard_map(
        work,
        mesh=torus,
        in_specs=(
            P("fs", None),
            P("fs", None),
            P("fs", None),
            P("fs"),
            P(None, "fs", TP),
            P(None, "fs", TP),
            P(None, "fs", TP),
        ),
        out_specs=(P("fs", None, TP), P("fs", None, TP), P("fs", None, TP), P("fs", TP)),
        check_vma=False,
    )
```
